1024 devices in a mesh: fs: 64 (over z, y), tp: 16 (over x, core).
Axes of the slice: x: 8, y: 8, z: 8, core: 2. Of those that a mesh axis runs over, the one named last changes fastest.
Arguments:
- up_pre: bfloat16 [49152, 4096], P('fs', 'tp'), may hold values from -6 to 6
- gate_value: bfloat16 [49152, 4096], P('fs', 'tp'), may hold values from -6 to 6
- out_cotangent: bfloat16 [49152, 2048], P('fs', 'tp'), may hold values from -8 to 8
- down_weight: bfloat16 [2048, 4096], P('fs', 'tp'), may hold values from -0.09375 to 0.09375
- conv_weight: float32 [3, 4096], P(None, 'tp'), may hold values from -3.5 to 3.5
- conv_bias: float32 [4096], P('tp'), may hold values from -3 to 3
Outputs:
- up_grad: bfloat16 [49152, 4096], P('fs', 'tp')
- gate_grad: bfloat16 [49152, 4096], P('fs', 'tp')
- weight_grad: float32 [2048, 4096], P('fs', 'tp')
- tap_grad: float32 [3, 4096], P(None, 'tp')
- bias_grad: float32 [4096], P('tp')
- unit_norms: float32 [4096], P('tp')
The draws below stay inside these ranges and needn't reach their ends.
All inputs are finite; a program needn't handle non-finite values.
Results may differ from the reference program's by a relative error of at most 0.0034.
Values may be sent and summed in bfloat16 or wider, within the bound.
A program may use at most 32 MiB of HBM per device.

```python
import jax
import jax.numpy as jnp

D = 2048
FF = 4096
TAPS = 3
TOKENS = 49152


def raised(values, stream_key, source, target, shards_of, factor):
    owner, partner = [(jnp.arange(values.shape[position]) // (values.shape[position] // shards_of)).reshape([-1 if axis == position else 1 for axis in range(values.ndim)]) for position in (source, target)]
    chosen = jax.random.permutation(stream_key, shards_of)[partner]
    strong = (owner == chosen) | (owner == (partner + shards_of // 2) % shards_of)
    return jnp.where(strong, factor * values, values)


def level_of(key, dims, shards, least, largest):
    gain = 1.0
    for dim, shards_of in shards:
        heights = jax.random.uniform(jax.random.fold_in(jax.random.fold_in(key, 6), dim), (shards_of,), jnp.float32, least / len(shards), largest / len(shards))
        gain = gain * jnp.repeat(jnp.exp(heights), dims[dim] // shards_of).reshape((-1,) + (1,) * (len(dims) - 1 - dim))
    return gain


def noise(rng, shape, spread, reach, split=(), kind=jnp.bfloat16):
    drawn = spread * jax.random.normal(rng, shape, jnp.float32)
    if split:
        drawn = drawn * level_of(rng, shape, split, -0.22, 0.18)
    return jnp.clip(drawn, -reach, reach).astype(kind)


def heavy_noise(own_key, dims, spread, limit, pieces, heavy, held_as=jnp.bfloat16):
    drawn = spread * jax.random.normal(own_key, dims, jnp.float32)
    if pieces:
        drawn = drawn * level_of(own_key, dims, pieces, -0.22, 0.18)
    return jnp.clip(raised(drawn, jax.random.fold_in(own_key, 3), *heavy), -limit, limit).astype(held_as)


def setup_inputs(seed: int = 0) -> dict:
    seeds = jax.random.split(jax.random.key(seed), 7)
    up_pre = noise(seeds[0], (TOKENS, FF), 1.0, 6.0, ((0, 64), (1, 16)))
    gate_value = noise(seeds[1], (TOKENS, FF), 1.0, 6.0, ((0, 64), (1, 16)))
    out_cotangent = heavy_noise(seeds[2], (TOKENS, D), 1.0, 8.0, ((0, 64), (1, 16)), (0, 1, 64, 4.0))
    down_weight = noise(seeds[3], (D, FF), FF ** -0.5, 0.09375, ((0, 64), (1, 16)))
    conv_weight = noise(seeds[4], (TAPS, FF), TAPS ** -0.5, 3.5, ((1, 16),), jnp.float32)
    conv_bias = noise(seeds[5], (FF,), 0.5, 3.0, ((0, 16),), jnp.float32)
    return dict(up_pre=up_pre, gate_value=gate_value, out_cotangent=out_cotangent, down_weight=down_weight, conv_weight=conv_weight, conv_bias=conv_bias)


def reference(up_pre, gate_value, out_cotangent, down_weight, conv_weight, conv_bias):
    padded = jnp.pad(up_pre.astype(jnp.float32), ((TAPS - 1, 0), (0, 0)))
    conv_out = jnp.zeros((TOKENS, FF), jnp.float32) + conv_bias[None, :]
    for tap_index in range(TAPS):
        conv_out = conv_out + conv_weight[tap_index][None, :] * padded[tap_index:tap_index + TOKENS]
    sigmoid_val = jax.nn.sigmoid(conv_out)
    activated = conv_out * sigmoid_val
    gate_float = gate_value.astype(jnp.float32)
    hidden = (activated * gate_float).astype(jnp.bfloat16)
    hidden_grad = jnp.dot(out_cotangent, down_weight, preferred_element_type=jnp.float32)
    gate_grad = (hidden_grad * activated).astype(jnp.bfloat16)
    conv_grad = hidden_grad * gate_float * sigmoid_val * (1.0 + conv_out * (1.0 - sigmoid_val))
    after = jnp.pad(conv_grad, ((0, TAPS - 1), (0, 0)))
    up_grad = jnp.zeros((TOKENS, FF), jnp.float32)
    for tap_index in range(TAPS):
        lead = TAPS - 1 - tap_index
        up_grad = up_grad + conv_weight[tap_index][None, :] * after[lead:lead + TOKENS]
    tap_grad = jnp.stack([jnp.sum(conv_grad * padded[tap_index:tap_index + TOKENS], axis=0)
                          for tap_index in range(TAPS)])
    bias_grad = jnp.sum(conv_grad, axis=0)
    weight_grad = jnp.dot(out_cotangent.T, hidden, preferred_element_type=jnp.float32)
    unit_norms = jnp.sum(weight_grad * weight_grad, axis=0)
    return (up_grad.astype(jnp.bfloat16), gate_grad, weight_grad, tap_grad, bias_grad, unit_norms)
```

```python
import functools

import jax
import jax.numpy as jnp
from jax import lax
from jax.experimental import pallas as pl
from jax.experimental.pallas import tpu as pltpu
from jax.sharding import PartitionSpec as P

MESH = pl.DeviceIdType.MESH
BF16 = jnp.bfloat16
F32 = jnp.float32


def ring_offsets(n):
    half = n // 2
    return [o for d in range(1, half + 1) for o in ((d, -d) if 2 * d < n else (d,))]


RELAY = {3: 2, 4: 2, -3: -2}


def kernel(dims, up, gate, cot, w, cw, cb, upg, gg, wg, tap, bias, nrm, *s):
    nx, ny, nz = dims
    (cot_all, wall, upf, act, dact, hid, hg, cgp, partf, partb, recv_a, send_b, recv_f,
     zsend, zrecv, zown, halo_up, halo_cg, ty, tz, qy, qz,
     x_s, x_r, sib_s, sib_r, wy_s, wy_r, wz_s, wz_r, a_s, a_r, f_s, f_r, z_s, z_r,
     h_s, h_r, ty_s, ty_r, tz_s, tz_r, qy_s, qy_r, qz_s, qz_r) = s
    tokens, width = up.shape
    half_t = tokens // 2
    tile = min(96, tokens // 2)
    hx, hz = nx // 2, nz // 2
    fs, tp = lax.axis_index("fs"), lax.axis_index("tp")
    x, c = lax.div(tp, 2), lax.rem(tp, 2)
    z, y = lax.div(fs, ny), lax.rem(fs, ny)

    def wrap(v, n):
        return lax.rem(v + 2 * n, n)

    def dev(x_=x, c_=c, y_=y, z_=z):
        return {"fs": z_ * ny + y_, "tp": x_ * 2 + c_}

    def flat(step):
        other = wrap(fs + step, ny * nz)
        return {"fs": other, "tp": tp}

    sends = []

    def rcopy(src, dst, ss, rs, to):
        return pltpu.make_async_remote_copy(
            src_ref=src, dst_ref=dst, send_sem=ss, recv_sem=rs, device_id=to, device_id_type=MESH
        )

    def send(src, dst, ss, rs, to):
        copy = rcopy(src, dst, ss, rs, to)
        copy.start()
        sends.append(copy)

    def arrived(dst, ss, rs, to):
        rcopy(dst, dst, ss, rs, to).wait_recv()

    sibling = dev(c_=1 - c)
    x_to = (dev(x_=wrap(x + 1, nx)), dev(x_=wrap(x - 1, nx)))
    z_to = (dev(z_=wrap(z + 1, nz)), dev(z_=wrap(z - 1, nz)))
    y_offs = ring_offsets(ny)
    relayed = [o for o in y_offs if o in RELAY]
    hubs = sorted({RELAY[o] for o in relayed})
    finals = [o for o in y_offs if o not in RELAY]

    barrier = pltpu.get_barrier_semaphore()
    peers = [sibling, *x_to, flat(1), flat(-1)]
    peers += [dev(y_=wrap(y + j, ny)) for j in range(1, ny)]
    peers += [dev(z_=wrap(z + j, nz)) for j in range(1, nz)]
    for peer in peers:
        pl.semaphore_signal(barrier, inc=1, device_id=peer, device_id_type=MESH)
    pl.semaphore_wait(barrier, len(peers))

    for h in range(2):
        for way in range(2):
            if hx == 1 and h != way:
                continue
            send(cot.at[pl.ds(h * half_t, half_t)], cot_all.at[x, c, h],
                 x_s.at[way, 0, h], x_r.at[way, 0, h], x_to[way])
    send(up.at[pl.ds(tokens - 16, 16)], halo_up, h_s.at[0], h_r.at[0], flat(1))
    for j in range(1, ny):
        send(w, wall.at[z, y], wy_s.at[j - 1], wy_r.at[j - 1], dev(y_=wrap(y + j, ny)))
    for h in range(2):
        send(cot.at[pl.ds(h * half_t, half_t)], cot_all.at[x, c, h],
             sib_s.at[0, 0, h], sib_r.at[0, 0, h], sibling)
    wall[z, y] = w[...]
    for h in range(2):
        cot_all[x, c, h] = cot[pl.ds(h * half_t, half_t), :]

    taps = [cw[pl.ds(k, 1), :] for k in range(3)]
    bias_row = cb[...]

    def widen(i, carry):
        base = pl.multiple_of(i * tile, 16)
        upf[pl.ds(base + 8, tile), :] = up[pl.ds(base, tile), :].astype(F32)
        return carry

    lax.fori_loop(0, tokens // tile, widen, 0)

    def shifted_up(base):
        rows = upf[pl.ds(base, tile + 8), :]
        return [rows[6 + k : 6 + k + tile] for k in range(3)]

    def forward(i, carry):
        base = pl.multiple_of(i * tile, 16)
        conv = bias_row
        for k, rows in enumerate(shifted_up(base)):
            conv = conv + taps[k] * rows
        sig = 1.0 / (1.0 + jnp.exp(-conv))
        gate_f = gate[pl.ds(base, tile), :].astype(F32)
        activated = conv * sig
        act[pl.ds(base, tile), :] = activated
        dact[pl.ds(base, tile), :] = gate_f * sig * (1.0 + conv * (1.0 - sig))
        hid[pl.ds(base, tile), :] = (activated * gate_f).astype(BF16)
        return carry

    lax.fori_loop(1, tokens // tile, forward, 0)
    arrived(halo_up, h_s.at[0], h_r.at[0], flat(1))
    upf[0:8, :] = jnp.where(fs > 0, halo_up[...].astype(F32)[8:16], 0.0)
    forward(0, 0)

    for j in range(1, ny):
        arrived(wall.at[z, wrap(y - j, ny)], wy_s.at[j - 1], wy_r.at[j - 1], sibling)
    half_y = ny // 2

    def w_piece(z_, h):
        return wall.at[z_, pl.ds(h * half_y, half_y)]

    def w_send(way, step, h):
        if step >= hz or (step == hz - 1 and h != way):
            return
        piece = w_piece(wrap(z - step if way == 0 else z + step, nz), h)
        send(piece, piece, wz_s.at[way, step, h], wz_r.at[way, step, h], z_to[way])

    def w_arrive(way, d, h):
        if d == hz and h != way:
            return
        piece = w_piece(wrap(z - d if way == 0 else z + d, nz), h)
        arrived(piece, wz_s.at[way, d - 1, h], wz_r.at[way, d - 1, h], z_to[way])
        w_send(way, d, h)

    for h in range(2):
        for way in range(2):
            w_send(way, 0, h)

    def origin(k):
        d = (k + 1) // 2
        return wrap(x - d if (k % 2 == 1 or d == hx) else x + d, nx)

    def wgrad(k):
        org = origin(k)
        for cc in range(2):
            block = cot_all[org, cc].reshape(tokens, cot.shape[1])
            part = lax.dot_general(block, hid[...], (((0,), (0,)), ((), ())),
                                   preferred_element_type=F32)
            part = part.reshape(half_y, w.shape[0], width)
            partf[k, pl.ds(cc * half_y, half_y)] = part
            partb[k, pl.ds(cc * half_y, half_y)] = part.astype(BF16)

    def rs_first(k):
        for o in y_offs:
            target = wrap(y - o, ny)
            if o in RELAY:
                i = relayed.index(o)
                send(partb.at[k, target], recv_a.at[k, i], a_s.at[k, i], a_r.at[k, i],
                     dev(y_=wrap(y - o + RELAY[o], ny)))
            elif o not in hubs:
                i = finals.index(o)
                send(partb.at[k, target], recv_f.at[k, i], f_s.at[k, i], f_r.at[k, i],
                     dev(y_=target))

    def rs_second(k):
        for b, r in enumerate(hubs):
            target = wrap(y - r, ny)
            total = partf[k, target]
            for i, o in enumerate(relayed):
                if RELAY[o] == r:
                    arrived(recv_a.at[k, i], a_s.at[k, i], a_r.at[k, i], sibling)
                    total = total + recv_a[k, i].astype(F32)
            send_b[k, b] = total.astype(BF16)
            i = finals.index(r)
            send(send_b.at[k, b], recv_f.at[k, i], f_s.at[k, i], f_r.at[k, i], dev(y_=target))

    def z_copy(k):
        org = origin(k)
        slot = wrap(z - org - 1, nz)
        return rcopy(zsend.at[k], zrecv.at[slot], z_s.at[k], z_r.at[slot], dev(z_=org))

    def rs_third(k):
        total = partf[k, y]
        for i in range(len(finals)):
            arrived(recv_f.at[k, i], f_s.at[k, i], f_r.at[k, i], sibling)
            total = total + recv_f[k, i].astype(F32)

        @pl.when(origin(k) == z)
        def _():
            zown[...] = total

        @pl.when(origin(k) != z)
        def _():
            zsend[k] = total.astype(BF16)
            z_copy(k).start()

    def chunks(d):
        return [k for k in range(nx) if (k + 1) // 2 == d]

    for h in range(2):
        arrived(cot_all.at[x, 1 - c, h], sib_s.at[0, 0, h], sib_r.at[0, 0, h], sibling)
    wgrad(0)
    rs_first(0)

    def grad_hidden(j, carry):
        org = wrap(x - hx + 1 + j, nx)
        weights = wall[org].reshape(ny * w.shape[0], width)
        for h in range(2):
            rows = jnp.concatenate([cot_all[org, 0, h], cot_all[org, 1, h]], axis=-1)
            hg[h] += jnp.dot(rows, weights, preferred_element_type=F32)
        return carry

    hg[...] = jnp.zeros_like(hg)

    for d in range(1, hx + 1):
        if d == hx:
            for dd in range(d, hz + 1):
                for h in range(2):
                    for way in range(2):
                        w_arrive(way, dd, h)
            lax.fori_loop(0, nx - 1, grad_hidden, 0)
        for h in range(2):
            for way in range(2):
                if d == hx and h != way:
                    continue
                org = wrap(x - d if way == 0 else x + d, nx)
                piece = cot_all.at[org, c, h]
                arrived(piece, x_s.at[way, d - 1, h], x_r.at[way, d - 1, h], x_to[way])
                if d < hx and not (d == hx - 1 and h != way):
                    send(piece, piece, x_s.at[way, d, h], x_r.at[way, d, h], x_to[way])
                send(piece, piece, sib_s.at[way, d, h], sib_r.at[way, d, h], sibling)
            if d < hx:
                for way in range(2):
                    w_arrive(way, d, h)
        for k in chunks(d - 1):
            rs_second(k)
        if d >= 2:
            for k in chunks(d - 2):
                rs_third(k)
        for h in range(2):
            for way in range(2):
                if d == hx and h != way:
                    continue
                org = wrap(x - d if way == 0 else x + d, nx)
                arrived(cot_all.at[org, 1 - c, h], sib_s.at[way, d, h], sib_r.at[way, d, h], sibling)
        for k in chunks(d):
            wgrad(k)
            rs_first(k)

    grad_hidden(nx - 1, 0)
    rows_h = half_t // tile

    def eight(v):
        return jnp.sum(v.reshape(tile // 8, 8, width), axis=0)

    def backward(i, sums):
        base = pl.multiple_of(i * tile, 16)
        grad = hg[lax.div(i, rows_h), pl.ds(pl.multiple_of(lax.rem(i, rows_h) * tile, 16), tile), :]
        gg[pl.ds(base, tile), :] = (grad * act[pl.ds(base, tile), :]).astype(BF16)
        conv_grad = grad * dact[pl.ds(base, tile), :]
        cgp[pl.ds(base, tile), :] = conv_grad
        ups = shifted_up(base)
        return tuple(sums[k] + eight(conv_grad * ups[k]) for k in range(3)) + (
            sums[3] + eight(conv_grad),
        )

    zero = jnp.zeros((8, width), F32)
    sums = backward(0, (zero,) * 4)
    send(cgp.at[pl.ds(0, 8)], halo_cg, h_s.at[1], h_r.at[1], flat(-1))
    sums = lax.fori_loop(1, tokens // tile, backward, sums)
    for k in chunks(hx - 1):
        rs_third(k)
    for k in chunks(hx):
        rs_second(k)
    row = jnp.concatenate([jnp.sum(v, axis=0, keepdims=True) for v in sums], axis=0)
    ty[y] = row
    for j in range(1, ny):
        send(ty.at[y], ty.at[y], ty_s.at[j - 1], ty_r.at[j - 1], dev(y_=wrap(y + j, ny)))

    def up_grads(i, carry):
        base = pl.multiple_of(i * tile, 16)
        rows = cgp[pl.ds(base, tile + 8), :]
        total = taps[0] * rows[2 : 2 + tile] + taps[1] * rows[1 : 1 + tile] + taps[2] * rows[0:tile]
        upg[pl.ds(base, tile), :] = total.astype(BF16)
        return carry

    lax.fori_loop(0, tokens // tile - 1, up_grads, 0)
    for k in chunks(hx):
        rs_third(k)
    arrived(halo_cg, h_s.at[1], h_r.at[1], flat(-1))
    cgp[pl.ds(tokens, 8), :] = jnp.where(fs < ny * nz - 1, halo_cg[...], 0.0)
    up_grads(tokens // tile - 1, 0)

    def gather(buf, n, me, ss, rs, first):
        if first:
            for j in range(1, n):
                to = dev(y_=wrap(y + j, ny)) if buf is ty or buf is qy else dev(z_=wrap(z + j, nz))
                send(buf.at[me], buf.at[me], ss.at[j - 1], rs.at[j - 1], to)
            return None
        for j in range(1, n):
            arrived(buf.at[wrap(me - j, n)], ss.at[j - 1], rs.at[j - 1], sibling)
        total = buf[0]
        for j in range(1, n):
            total = total + buf[j]
        return total

    tz[z] = gather(ty, ny, y, ty_s, ty_r, False)
    gather(tz, nz, z, tz_s, tz_r, True)

    total = zown[...]
    for j in range(nz - 1):
        arrived(zrecv.at[j], z_s.at[0], z_r.at[j], sibling)
    for j in range(nz - 1):
        total = total + zrecv[j].astype(F32)
    wg[...] = total
    qy[y] = jnp.sum(total * total, axis=0, keepdims=True)
    gather(qy, ny, y, qy_s, qy_r, True)
    taps_total = gather(tz, nz, z, tz_s, tz_r, False)
    tap[...] = taps_total[0:3]
    bias[...] = taps_total[3:4]
    qz[z] = gather(qy, ny, y, qy_s, qy_r, False)
    gather(qz, nz, z, qz_s, qz_r, True)
    nrm[...] = gather(qz, nz, z, qz_s, qz_r, False)

    for copy in sends:
        copy.wait_send()
    for k in range(nx):

        @pl.when(origin(k) != z)
        def _(k=k):
            z_copy(k).wait_send()


def per_device(dims, up_pre, gate_value, out_cotangent, down_weight, conv_weight, conv_bias):
    nx, ny, nz = dims
    tokens, width = up_pre.shape
    depth, rows = out_cotangent.shape[1], down_weight.shape[0]
    hx, hz = nx // 2, nz // 2
    y_offs = ring_offsets(ny)
    n_rel = max(1, len([o for o in y_offs if o in RELAY]))
    n_fin = len([o for o in y_offs if o not in RELAY])
    vmem, dma = pltpu.VMEM, pltpu.SemaphoreType.DMA
    scratch = [
        vmem((nx, 2, 2, tokens // 2, depth), BF16),
        vmem((nz, ny, rows, width), BF16),
        vmem((tokens + 8, width), F32),
        vmem((tokens, width), F32),
        vmem((tokens, width), F32),
        vmem((tokens, width), BF16),
        vmem((2, tokens // 2, width), F32),
        vmem((tokens + 8, width), F32),
        vmem((nx, ny, rows, width), F32),
        vmem((nx, ny, rows, width), BF16),
        vmem((nx, n_rel, rows, width), BF16),
        vmem((nx, 2, rows, width), BF16),
        vmem((nx, n_fin, rows, width), BF16),
        vmem((nx, rows, width), BF16),
        vmem((nz - 1, rows, width), BF16),
        vmem((rows, width), F32),
        vmem((16, width), BF16),
        vmem((8, width), F32),
        vmem((ny, 4, width), F32),
        vmem((nz, 4, width), F32),
        vmem((ny, 1, width), F32),
        vmem((nz, 1, width), F32),
        dma((2, hx, 2)), dma((2, hx, 2)),
        dma((2, hx + 1, 2)), dma((2, hx + 1, 2)),
        dma((ny - 1,)), dma((ny - 1,)),
        dma((2, hz, 2)), dma((2, hz, 2)),
        dma((nx, n_rel)), dma((nx, n_rel)),
        dma((nx, n_fin)), dma((nx, n_fin)),
        dma((nx,)), dma((nz - 1,)),
        dma((2,)), dma((2,)),
        dma((ny - 1,)), dma((ny - 1,)),
        dma((nz - 1,)), dma((nz - 1,)),
        dma((ny - 1,)), dma((ny - 1,)),
        dma((nz - 1,)), dma((nz - 1,)),
    ]
    spec = pl.BlockSpec(memory_space=pltpu.VMEM)
    up_grad, gate_grad, weight_grad, tap_grad, bias_grad, unit_norms = pl.pallas_call(
        functools.partial(kernel, dims),
        out_shape=(
            jax.ShapeDtypeStruct((tokens, width), BF16),
            jax.ShapeDtypeStruct((tokens, width), BF16),
            jax.ShapeDtypeStruct((rows, width), F32),
            jax.ShapeDtypeStruct((3, width), F32),
            jax.ShapeDtypeStruct((1, width), F32),
            jax.ShapeDtypeStruct((1, width), F32),
        ),
        in_specs=[spec] * 6,
        out_specs=(spec,) * 6,
        scratch_shapes=scratch,
        compiler_params=pltpu.CompilerParams(
            collective_id=0, has_side_effects=True, vmem_limit_bytes=40 * 1024 * 1024
        ),
    )(up_pre, gate_value, out_cotangent, down_weight, conv_weight, conv_bias[None])
    return up_grad, gate_grad, weight_grad, tap_grad, bias_grad[0], unit_norms[0]


def solution(mesh):
    nx = mesh.shape["tp"] // 2
    dims = (nx, mesh.shape["fs"] // nx, nx)
    return jax.shard_map(
        functools.partial(per_device, dims),
        mesh=mesh,
        in_specs=(P("fs", "tp"), P("fs", "tp"), P("fs", "tp"), P("fs", "tp"), P(None, "tp"), P("tp")),
        out_specs=(P("fs", "tp"), P("fs", "tp"), P("fs", "tp"), P(None, "tp"), P("tp"), P("tp")),
        check_vma=False,
    )
```

```python
import functools

import jax
import jax.numpy as jnp
from jax import lax
from jax.experimental import pallas as pl
from jax.experimental.pallas import tpu as pltpu
from jax.sharding import PartitionSpec as P

MESH = pl.DeviceIdType.MESH
BF16 = jnp.bfloat16
F32 = jnp.float32


def ring_offsets(n):
    half = n // 2
    return [o for d in range(1, half + 1) for o in ((d, -d) if 2 * d < n else (d,))]


RELAY = {3: 2, 4: 2, -3: -2}


def kernel(dims, up_in, gate_in, cot_in, w_in, cw_in, cb_in, upg, gg, wg, tap, bias, nrm, *s):
    nx, ny, nz = dims
    (cot_all, wall, upf, act, dact, hid, hg, cgp, partf, partb, recv_a, send_b, recv_f,
     zsend, zrecv, zown, halo_up, halo_cg, ty, tz, qy, qz, up, gate, cw, cb,
     in_s, x_s, x_r, sib_s, sib_r, wy_s, wy_r, wz_s, wz_r, a_s, a_r, f_s, f_r, z_s, z_r,
     h_s, h_r, sum_s, sum_r) = s
    tokens, width = up_in.shape
    depth, n_rows = cot_in.shape[1], w_in.shape[0]
    half_t, half_y = tokens // 2, ny // 2
    tile = min(96, tokens // 2)
    tiles = tokens // tile
    hx, hz = nx // 2, nz // 2
    fs, tp = lax.axis_index("fs"), lax.axis_index("tp")
    x, c = lax.div(tp, 2), lax.rem(tp, 2)
    z, y = lax.div(fs, ny), lax.rem(fs, ny)

    def wrap(v, n):
        return lax.rem(v + 2 * n, n)

    def dev(x_=x, c_=c, y_=y, z_=z):
        return {"fs": z_ * ny + y_, "tp": x_ * 2 + c_}

    def flat(step):
        return {"fs": wrap(fs + step, ny * nz), "tp": tp}

    sibling = dev(c_=1 - c)
    x_to = (dev(x_=wrap(x + 1, nx)), dev(x_=wrap(x - 1, nx)))
    z_to = (dev(z_=wrap(z + 1, nz)), dev(z_=wrap(z - 1, nz)))

    def rcopy(src, dst, ss, rs, to):
        return pltpu.make_async_remote_copy(
            src_ref=src, dst_ref=dst, send_sem=ss, recv_sem=rs, device_id=to, device_id_type=MESH
        )

    def send(src, dst, ss, rs, to):
        rcopy(src, dst, ss, rs, to).start()

    def arrived(size_of, rs):
        rcopy(size_of, size_of, x_s.at[0], rs, sibling).wait_recv()

    def sent(size_of, ss):
        rcopy(size_of, size_of, ss, z_r.at[0], sibling).wait_send()

    def load(src, dst, i):
        copy = pltpu.make_async_copy(src, dst, in_s.at[i])
        copy.start()
        return copy

    cot_loads = [
        load(cot_in.at[pl.ds(h * half_t, half_t)], cot_all.at[x, c, h], h) for h in range(2)
    ]
    w_load = load(w_in, wall.at[z, y], 2)
    up_load = load(up_in, up, 3)
    gate_load = load(gate_in, gate, 4)
    row_loads = [load(cw_in, cw, 5), load(cb_in, cb, 6)]

    barrier = pltpu.get_barrier_semaphore()
    peers = [sibling, *x_to, flat(1), flat(-1)]
    peers += [dev(y_=wrap(y + j, ny)) for j in range(1, ny)]
    peers += [dev(z_=wrap(z + j, nz)) for j in range(1, nz)]
    for peer in peers:
        pl.semaphore_signal(barrier, inc=1, device_id=peer, device_id_type=MESH)
    pl.semaphore_wait(barrier, len(peers))

    w_load.wait()
    for j in range(1, ny):
        send(wall.at[z, y], wall.at[z, y], wy_s.at[0], wy_r.at[0], dev(y_=wrap(y + j, ny)))

    def x_piece(way, d, j):
        return wrap(x - d if way == 0 else x + d, nx), (j if way == 0 else 1 - j)

    def x_send(way, d, j):
        if d < hx and not (d == hx - 1 and j == 1):
            org, h = x_piece(way, d, j)
            piece = cot_all.at[org, c, h]
            send(piece, piece, x_s.at[0], x_r.at[way, d, j], x_to[way])

    def x_step(d, j):
        for way in range(2):
            org, h = x_piece(way, d, j)
            piece = cot_all.at[org, c, h]
            arrived(piece, x_r.at[way, d - 1, j])
            x_send(way, d, j)
            send(piece, piece, sib_s.at[0], sib_r.at[d], sibling)

    for copy in cot_loads:
        copy.wait()
    for j in range(2):
        for way in range(2):
            x_send(way, 0, j)
    for h in range(2):
        send(cot_all.at[x, c, h], cot_all.at[x, c, h], sib_s.at[0], sib_r.at[0], sibling)
    up_load.wait()
    send(up.at[pl.ds(tokens - 16, 16)], halo_up, h_s.at[0], h_r.at[0], flat(1))
    gate_load.wait()
    for copy in row_loads:
        copy.wait()

    taps = [cw[pl.ds(k, 1), :] for k in range(3)]
    bias_row = cb[...]

    def widen(i, carry):
        base = pl.multiple_of(i * tile, 16)
        upf[pl.ds(base + 8, tile), :] = up[pl.ds(base, tile), :].astype(F32)
        return carry

    lax.fori_loop(0, tiles, widen, 0)

    def shifted_up(base):
        rows = upf[pl.ds(base, tile + 8), :]
        return [rows[6 + k : 6 + k + tile] for k in range(3)]

    def forward(i, carry):
        base = pl.multiple_of(i * tile, 16)
        conv = bias_row
        for k, rows in enumerate(shifted_up(base)):
            conv = conv + taps[k] * rows
        sig = 1.0 / (1.0 + jnp.exp(-conv))
        gate_f = gate[pl.ds(base, tile), :].astype(F32)
        activated = conv * sig
        act[pl.ds(base, tile), :] = activated
        dact[pl.ds(base, tile), :] = gate_f * sig * (1.0 + conv * (1.0 - sig))
        hid[pl.ds(base, tile), :] = (activated * gate_f).astype(BF16)
        return carry

    lax.fori_loop(1, tiles, forward, 0)
    arrived(halo_up, h_r.at[0])
    upf[0:8, :] = jnp.where(fs > 0, halo_up[...].astype(F32)[8:16], 0.0)
    forward(0, 0)

    def w_piece(way, d, j):
        h = j if way == 0 else 1 - j
        return wall.at[wrap(z - d if way == 0 else z + d, nz), pl.ds(h * half_y, half_y)]

    def w_send(way, d, j):
        if d < hz and not (d == hz - 1 and j == 1):
            piece = w_piece(way, d, j)
            send(piece, piece, wz_s.at[0], wz_r.at[way, d, j], z_to[way])

    w_left = [(d, j) for d in range(1, hz + 1) for j in range(2) if not (d == hz and j == 1)]

    def w_steps(count):
        for _ in range(min(count, len(w_left))):
            d, j = w_left.pop(0)
            for way in range(2):
                arrived(w_piece(way, d, j), wz_r.at[way, d - 1, j])
                w_send(way, d, j)

    def origin(k):
        d = (k + 1) // 2
        return wrap(x - d if (k % 2 == 1 or d == hx) else x + d, nx)

    def wgrad(k, cc):
        block = cot_all[origin(k), cc].reshape(tokens, depth)
        part = lax.dot_general(block, hid[...], (((0,), (0,)), ((), ())),
                               preferred_element_type=F32)
        part = part.reshape(half_y, n_rows, width)
        partf[k, pl.ds(cc * half_y, half_y)] = part
        partb[k, pl.ds(cc * half_y, half_y)] = part.astype(BF16)

    offsets = ring_offsets(ny)
    relayed = [o for o in offsets if o in RELAY]
    hubs = sorted({RELAY[o] for o in relayed})
    finals = [o for o in offsets if o not in RELAY]

    def turned(k, o):
        return o if k % 2 == 0 else -o

    def rs_first(k):
        for o in relayed:
            target, via = wrap(y - turned(k, o), ny), wrap(y - turned(k, o - RELAY[o]), ny)
            send(partb.at[k, target], recv_a.at[k, relayed.index(o)], a_s.at[0], a_r.at[k],
                 dev(y_=via))
        for i, o in enumerate(finals):
            if o not in hubs:
                target = wrap(y - turned(k, o), ny)
                send(partb.at[k, target], recv_f.at[k, i], f_s.at[0], f_r.at[k], dev(y_=target))

    def rs_second(k):
        if relayed:
            arrived(recv_a.at[k], a_r.at[k])
        for b, r in enumerate(hubs):
            target = wrap(y - turned(k, r), ny)
            total = partf[k, target]
            for i, o in enumerate(relayed):
                if RELAY[o] == r:
                    total = total + recv_a[k, i].astype(F32)
            send_b[k, b] = total.astype(BF16)
            send(send_b.at[k, b], recv_f.at[k, finals.index(r)], f_s.at[0], f_r.at[k],
                 dev(y_=target))

    def rs_third(k):
        org = origin(k)
        arrived(recv_f.at[k], f_r.at[k])
        total = partf[k, y]
        for i in range(len(finals)):
            total = total + recv_f[k, i].astype(F32)

        @pl.when(org == z)
        def _():
            zown[...] = total

        @pl.when(org != z)
        def _():
            zsend[k] = total.astype(BF16)
            send(zsend.at[k], zrecv.at[wrap(z - org - 1, nz)], z_s.at[0], z_r.at[0], dev(z_=org))

    def chunks(d):
        return [k for k in range(nx) if (k + 1) // 2 == d]

    left = {"second": 0, "third": 0}

    def reduce_steps(second, third):
        while left["second"] <= min(second, hx):
            for k in chunks(left["second"]):
                rs_second(k)
            left["second"] += 1
        while left["third"] <= min(third, hx):
            for k in chunks(left["third"]):
                rs_third(k)
            left["third"] += 1

    def own_chunks(d):
        for k in chunks(d):
            wgrad(k, c)
        arrived(cot_all.at[pl.ds(0, len(chunks(d))), 0], sib_r.at[d])
        for k in chunks(d):
            wgrad(k, 1 - c)
            rs_first(k)

    x_step(1, 0)
    arrived(wall.at[z, pl.ds(0, ny - 1)], wy_r.at[0])
    for j in range(2):
        for way in range(2):
            w_send(way, 0, j)
    own_chunks(0)
    for d in range(1, hx):
        x_step(d, 1)
        if d >= 2:
            w_steps(1)
            reduce_steps(d - 2, d - 3)
        if d < hx - 1:
            x_step(d + 1, 0)
        own_chunks(d)
        if d < hx - 1:
            w_steps(1)
    if hx > 1:
        x_step(hx, 0)
    own_chunks(hx)

    w_steps(1)
    reduce_steps(hx - 2, hx - 3)
    w_steps(1)

    hg[...] = jnp.zeros_like(hg)

    def grad_hidden(org, carry):
        weights = wall[org].reshape(ny * n_rows, width)
        for h in range(2):
            rows = jnp.concatenate([cot_all[org, 0, h], cot_all[org, 1, h]], axis=-1)
            hg[h] += jnp.dot(rows, weights, preferred_element_type=F32)
        return carry

    def grad_hidden_near(e, carry):
        return grad_hidden(wrap(z - hz + 1 + e, nz), carry)

    lax.fori_loop(0, nz - 1, grad_hidden_near, 0)
    reduce_steps(hx - 1, hx - 2)
    reduce_steps(hx, hx - 2)
    w_steps(len(w_left))
    grad_hidden(wrap(z + hz, nz), 0)
    rows_h = half_t // tile

    def eight(v):
        return jnp.sum(v.reshape(tile // 8, 8, width), axis=0)

    def backward(i, sums):
        base = pl.multiple_of(i * tile, 16)
        grad = hg[lax.div(i, rows_h), pl.ds(pl.multiple_of(lax.rem(i, rows_h) * tile, 16), tile), :]
        gg[pl.ds(base, tile), :] = (grad * act[pl.ds(base, tile), :]).astype(BF16)
        conv_grad = grad * dact[pl.ds(base, tile), :]
        cgp[pl.ds(base, tile), :] = conv_grad
        ups = shifted_up(base)
        return tuple(sums[k] + eight(conv_grad * ups[k]) for k in range(3)) + (
            sums[3] + eight(conv_grad),
        )

    zero = jnp.zeros((8, width), F32)
    sums = backward(0, (zero,) * 4)
    send(cgp.at[pl.ds(0, 8)], halo_cg, h_s.at[1], h_r.at[1], flat(-1))
    reduce_steps(hx, hx - 1)
    sums = lax.fori_loop(1, tiles, backward, sums)
    row = jnp.concatenate([jnp.sum(v, axis=0, keepdims=True) for v in sums], axis=0)

    sum_bufs = (ty, tz, qy, qz)

    def share(i, value):
        buf, n, me = sum_bufs[i], (ny, nz)[i % 2], (y, z)[i % 2]
        buf[me] = value
        for j in range(1, n):
            to = dev(y_=wrap(y + j, ny)) if i % 2 == 0 else dev(z_=wrap(z + j, nz))
            send(buf.at[me], buf.at[me], sum_s.at[i], sum_r.at[i], to)

    def shared_total(i):
        buf, n = sum_bufs[i], (ny, nz)[i % 2]
        arrived(buf.at[pl.ds(0, n - 1)], sum_r.at[i])
        total = buf[0]
        for j in range(1, n):
            total = total + buf[j]
        return total

    share(0, row)
    reduce_steps(hx, hx)

    def up_grads(i, carry):
        base = pl.multiple_of(i * tile, 16)
        rows = cgp[pl.ds(base, tile + 8), :]
        total = taps[0] * rows[2 : 2 + tile] + taps[1] * rows[1 : 1 + tile] + taps[2] * rows[0:tile]
        upg[pl.ds(base, tile), :] = total.astype(BF16)
        return carry

    lax.fori_loop(0, tiles - 1, up_grads, 0)
    arrived(halo_cg, h_r.at[1])
    cgp[pl.ds(tokens, 8), :] = jnp.where(fs < ny * nz - 1, halo_cg[...], 0.0)
    up_grads(tiles - 1, 0)
    share(1, shared_total(0))

    arrived(zrecv, z_r.at[0])
    total = zown[...]
    for j in range(nz - 1):
        total = total + zrecv[j].astype(F32)
    wg[...] = total
    share(2, jnp.sum(total * total, axis=0, keepdims=True))
    taps_total = shared_total(1)
    tap[...] = taps_total[0:3]
    bias[...] = taps_total[3:4]
    share(3, shared_total(2))
    sent(cot_all.at[pl.ds(0, nx - 1), 0], x_s.at[0])
    sent(cot_all.at[:, 0], sib_s.at[0])
    sent(wall.at[0, pl.ds(0, ny - 1)], wy_s.at[0])
    sent(wall.at[pl.ds(0, nz - 1)], wz_s.at[0])
    if relayed:
        sent(recv_a, a_s.at[0])
    sent(recv_f, f_s.at[0])
    sent(zrecv, z_s.at[0])
    sent(halo_up, h_s.at[0])
    sent(halo_cg, h_s.at[1])
    for i in range(3):
        sent(sum_bufs[i].at[pl.ds(0, (ny, nz)[i % 2] - 1)], sum_s.at[i])
    nrm[...] = shared_total(3)
    sent(qz.at[pl.ds(0, nz - 1)], sum_s.at[3])


def store(*refs):
    sources, targets, sem = refs[:6], refs[6:12], refs[12]
    copies = [pltpu.make_async_copy(a, b, sem.at[i]) for i, (a, b) in enumerate(zip(sources, targets))]
    for copy in copies:
        copy.start()
    for copy in copies:
        copy.wait()


def per_device(dims, up_pre, gate_value, out_cotangent, down_weight, conv_weight, conv_bias):
    nx, ny, nz = dims
    tokens, width = up_pre.shape
    depth, rows = out_cotangent.shape[1], down_weight.shape[0]
    hx, hz = nx // 2, nz // 2
    y_offs = ring_offsets(ny)
    n_rel = max(1, len([o for o in y_offs if o in RELAY]))
    n_fin = len([o for o in y_offs if o not in RELAY])
    vmem, dma = pltpu.VMEM, pltpu.SemaphoreType.DMA
    scratch = [
        vmem((nx, 2, 2, tokens // 2, depth), BF16),
        vmem((nz, ny, rows, width), BF16),
        vmem((tokens + 8, width), F32),
        vmem((tokens, width), F32),
        vmem((tokens, width), F32),
        vmem((tokens, width), BF16),
        vmem((2, tokens // 2, width), F32),
        vmem((tokens + 8, width), F32),
        vmem((nx, ny, rows, width), F32),
        vmem((nx, ny, rows, width), BF16),
        vmem((nx, n_rel, rows, width), BF16),
        vmem((nx, 2, rows, width), BF16),
        vmem((nx, n_fin, rows, width), BF16),
        vmem((nx, rows, width), BF16),
        vmem((nz - 1, rows, width), BF16),
        vmem((rows, width), F32),
        vmem((16, width), BF16),
        vmem((8, width), F32),
        vmem((ny, 4, width), F32),
        vmem((nz, 4, width), F32),
        vmem((ny, 1, width), F32),
        vmem((nz, 1, width), F32),
        vmem((tokens, width), BF16),
        vmem((tokens, width), BF16),
        vmem((3, width), F32),
        vmem((1, width), F32),
        dma((7,)),
        dma((1,)), dma((2, hx, 2)),
        dma((1,)), dma((hx + 1,)),
        dma((1,)), dma((1,)),
        dma((1,)), dma((2, hz, 2)),
        dma((1,)), dma((nx,)),
        dma((1,)), dma((nx,)),
        dma((1,)), dma((1,)),
        dma((2,)), dma((2,)),
        dma((4,)), dma((4,)),
    ]
    spec = pl.BlockSpec(memory_space=pltpu.VMEM)
    hbm = pl.BlockSpec(memory_space=pltpu.HBM)
    shapes = (
        jax.ShapeDtypeStruct((tokens, width), BF16),
        jax.ShapeDtypeStruct((tokens, width), BF16),
        jax.ShapeDtypeStruct((rows, width), F32),
        jax.ShapeDtypeStruct((3, width), F32),
        jax.ShapeDtypeStruct((1, width), F32),
        jax.ShapeDtypeStruct((1, width), F32),
    )
    results = pl.pallas_call(
        functools.partial(kernel, dims),
        out_shape=shapes,
        in_specs=[hbm] * 6,
        out_specs=(spec,) * 6,
        scratch_shapes=scratch,
        compiler_params=pltpu.CompilerParams(
            collective_id=0, has_side_effects=True, vmem_limit_bytes=40 * 1024 * 1024
        ),
    )(*[pltpu.with_memory_space_constraint(v, pltpu.HBM) for v in (up_pre, gate_value, out_cotangent, down_weight, conv_weight, conv_bias[None])])
    up_grad, gate_grad, weight_grad, tap_grad, bias_grad, unit_norms = pl.pallas_call(
        store,
        out_shape=shapes,
        in_specs=[spec] * 6,
        out_specs=(hbm,) * 6,
        scratch_shapes=[dma((6,))],
        compiler_params=pltpu.CompilerParams(vmem_limit_bytes=4 * 1024 * 1024),
    )(*results)
    return up_grad, gate_grad, weight_grad, tap_grad, bias_grad[0], unit_norms[0]


def solution(mesh):
    nx = mesh.shape["tp"] // 2
    dims = (nx, mesh.shape["fs"] // nx, nx)
    return jax.shard_map(
        functools.partial(per_device, dims),
        mesh=mesh,
        in_specs=(P("fs", "tp"), P("fs", "tp"), P("fs", "tp"), P("fs", "tp"), P(None, "tp"), P("tp")),
        out_specs=(P("fs", "tp"), P("fs", "tp"), P("fs", "tp"), P(None, "tp"), P("tp"), P("tp")),
        check_vma=False,
    )
```
